32 devices in a mesh: sp: 8 (over z, y), tp: 4 (over x, core).
Axes of the slice: x: 2, y: 2, z: 4, core: 2. Of those that a mesh axis runs over, the one named last changes fastest.
Arguments:
- queries: bfloat16 [6144, 1024], P('sp', 'tp'), may hold values from -6 to 6
- keys: bfloat16 [6144, 1024], P('sp', 'tp'), may hold values from -6 to 6
- values: bfloat16 [6144, 2048], P('sp', 'tp'), may hold values from -6 to 6
- out_gate: bfloat16 [6144, 2048], P('sp', 'tp'), may hold values from -6 to 6
- input_gates: float32 [2, 4, 6144], P(None, 'tp', 'sp'), may hold values from -4 to 300
- forget_gates: float32 [2, 4, 6144], P(None, 'tp', 'sp'), may hold values from -1 to 16
- doc_ids: int32 [6144], P('sp'), may hold values from 0 to 3, never falling along the last dimension, each value on 1 to 3072 neighbouring positions
- head_gain: float32 [2048], P('tp'), may hold values from 0.1 to 1.9
- w_out: bfloat16 [2048, 2048], P('tp'), may hold values from -0.25 to 0.25
- resid: bfloat16 [6144, 2048], P(('sp', 'tp')), may hold values from -30 to 30
- norm_gain: float32 [2048], replicated, may hold values from 0.1 to 1.9
- w_up: bfloat16 [2048, 8192], P('sp', 'tp'), may hold values from -0.125 to 0.125
- w_down: bfloat16 [8192, 2048], P('tp', 'sp'), may hold values from -0.0625 to 0.0625
Outputs:
- layer_out: bfloat16 [6144, 2048], P(('sp', 'tp'))
The draws below stay inside these ranges and needn't reach their ends.
Inputs may be any that keep to these rules, and one draw needn't show every extreme that they name: `doc_ids`: document numbers never fall along the positions.
All inputs are finite; a program needn't handle non-finite values.
Results may differ from the reference program's by a relative error of at most 0.013.
Values may be sent and summed in bfloat16 or wider, within the bound.
A program may use at most 128 MiB of HBM per device.

```python
import math
import jax
import jax.numpy as jnp
import numpy as np
from jax import lax

D = 2048
HEADS = 4
DQK = 256
DV = 512
FF = 8192
TOK_DEV = 768
TOKENS = 6144
N_SP = 8


def draw_resid(key, part):
    keys = jax.random.split(key, 2)
    base = jax.random.normal(keys[0], (TOKENS, D), jnp.float32)
    rows = jnp.exp(jax.random.uniform(keys[1], (TOKENS, 1), jnp.float32, -1.2, 1.2))
    cols = jnp.exp(jnp.linspace(-0.9, 0.9, D, dtype=jnp.float32))[None, :]
    return jnp.clip(base * rows * cols, -30.0, 30.0).astype(jnp.bfloat16)


def draw_input_gates(key, part):
    keys = jax.random.split(key, 1)
    gates = jnp.clip(jax.random.normal(keys[0], (2, HEADS, TOKENS), jnp.float32), -4.0, 4.0)
    return gates


def draw_forget_gates(key, part):
    keys = jax.random.split(key, 6)
    share = 0.5
    slow = jax.random.uniform(keys[0], (2, HEADS, 1), jnp.float32) < share
    fast_rate = jnp.exp(jax.random.uniform(keys[1], (2, HEADS, 1), jnp.float32, jnp.log(1.0 / 100.0), jnp.log(1.0 / 30.0)))
    rate = jnp.where(slow, 0.3 / TOKENS, fast_rate)
    factor = jnp.exp(jax.random.uniform(keys[2], (2, HEADS, TOKENS // TOK_DEV), jnp.float32, -0.7, 0.7))
    factor = jnp.repeat(factor, TOK_DEV, axis=2)
    noise = jnp.clip(jax.random.normal(keys[3], (2, HEADS, TOKENS), jnp.float32), -3.0, 3.0)
    pre = -jnp.log(rate * factor) + noise
    spots = jax.random.randint(keys[4], (2, HEADS, 3), 0, TOKENS)
    hit = jnp.any(jnp.arange(TOKENS)[None, None, None, :] == spots[..., None], axis=2)
    drop = jax.random.uniform(keys[5], (2, HEADS, TOKENS), jnp.float32, 0.0, 1.4)
    return jnp.where(hit, drop, pre)


def shard_levels(stream_key, extent, cuts, least, high):
    def one(axis_at, shards_of):
        steps = jax.random.uniform(jax.random.fold_in(jax.random.fold_in(stream_key, 6), axis_at), (shards_of,), jnp.float32, least / len(cuts), high / len(cuts))
        return jnp.repeat(jnp.exp(steps), extent[axis_at] // shards_of).reshape((-1,) + (1,) * (len(extent) - axis_at - 1))

    gain = one(*cuts[0])
    for cut in cuts[1:]:
        gain = gain * one(*cut)
    return gain


def profile(amount, total, limit, skew):
    loads = [(1 << 20) // math.isqrt(rank ** skew) + 1 for rank in range(2, amount + 1)]
    rest, holding = total - limit - (amount - 1), [1] * (amount - 1)
    while rest > 0:
        candidates = [i for i in range(amount - 1) if holding[i] < limit]
        pool, budget = sum([loads[i] for i in candidates]), rest
        for i in candidates:
            addition = min(limit - holding[i], max(1, budget * loads[i] // pool), rest)
            holding[i] = holding[i] + addition
            rest = rest - addition
    return np.array([limit] + holding)


def uneven_parts(own_key, count, total, bound, lean):
    if count == 2:
        one = jax.random.randint(own_key, (), max(1, total - bound), min(bound, total - 1) + 1)
        return jnp.stack([one, total - one])
    tallies = jnp.asarray(profile(count, total, bound, lean), jnp.int32)
    pairs = (count - 1) // 2
    source_of, sink = tallies[1:1 + 2 * pairs:2], tallies[2:2 + 2 * pairs:2]
    room = jnp.minimum(source_of - 1, bound - sink)
    moved = jax.random.randint(jax.random.fold_in(own_key, 1), (pairs,), 0, 1 << 20) % (room + 1)
    tallies = tallies.at[1:1 + 2 * pairs:2].set(source_of - moved).at[2:2 + 2 * pairs:2].set(sink + moved)
    return tallies[jax.random.permutation(jax.random.fold_in(own_key, 2), count)]


def gaussian(key, shape, deviation, most, cuts=(), kind=jnp.bfloat16):
    entries = deviation * jax.random.normal(key, shape, jnp.float32)
    if cuts:
        entries = entries * shard_levels(key, shape, cuts, -0.22, 0.18)
    return jnp.clip(entries, -most, most).astype(kind)


def setup_inputs(seed: int = 0) -> dict:
    arg_keys = jax.random.split(jax.random.key(seed), 14)
    queries = gaussian(arg_keys[0], (TOKENS, HEADS * DQK), 1.0, 6.0, ((0, 8), (1, 4)))
    keys = gaussian(arg_keys[1], (TOKENS, HEADS * DQK), 1.0, 6.0, ((0, 8), (1, 4)))
    values = gaussian(arg_keys[2], (TOKENS, HEADS * DV), 1.0, 6.0, ((0, 8), (1, 4)))
    out_gate = gaussian(arg_keys[3], (TOKENS, HEADS * DV), 1.0, 6.0, ((0, 8), (1, 4)))
    input_gates = draw_input_gates(jax.random.fold_in(arg_keys[13], 71), 0)
    forget_gates = draw_forget_gates(jax.random.fold_in(arg_keys[13], 71), 0)
    doc_ids = jnp.searchsorted(jnp.cumsum(uneven_parts(arg_keys[6], N_SP // 2, TOKENS, 4 * TOK_DEV, 0)), jnp.arange(TOKENS), side="right").astype(jnp.int32)
    head_gain = jnp.clip(1.0 + 0.18 * jax.random.normal(arg_keys[7], (HEADS * DV,), jnp.float32), 0.1, 1.9)
    w_out = gaussian(arg_keys[8], (HEADS * DV, D), (HEADS * DV // 4) ** -0.5, 0.25, ((0, 4),))
    resid = draw_resid(jax.random.fold_in(arg_keys[13], 71), 0)
    norm_gain = jnp.clip(1.0 + 0.18 * jax.random.normal(arg_keys[10], (D,), jnp.float32), 0.1, 1.9)
    w_up = gaussian(arg_keys[11], (D, FF), D ** -0.5, 0.125, ((0, 8), (1, 4)))
    w_down = gaussian(arg_keys[12], (FF, D), FF ** -0.5, 0.0625, ((0, 4), (1, 8)))
    return dict(queries=queries, keys=keys, values=values, out_gate=out_gate, input_gates=input_gates, forget_gates=forget_gates, doc_ids=doc_ids, head_gain=head_gain, w_out=w_out, resid=resid, norm_gain=norm_gain, w_up=w_up, w_down=w_down)


eps = 1e-06
far_low = -1e+30

def summarize(keys_blk, values_blk, in_gate, forget_pre, doc_pos):
    logf = jax.nn.log_sigmoid(forget_pre)
    cum = jnp.cumsum(logf)
    length = keys_blk.shape[0]
    last_doc = doc_pos[length - 1]
    tail = doc_pos == last_doc
    total = cum[length - 1]
    exponent = jnp.where(tail, total - cum + in_gate, far_low)
    peak = jnp.max(exponent)
    scaled = jnp.exp(exponent - peak)
    weighted = (keys_blk.astype(jnp.float32) * scaled[:, None]).astype(jnp.bfloat16)
    memory = jnp.einsum('sd,sv->dv', weighted.astype(jnp.float32), values_blk.astype(jnp.float32))
    norm_keys = lax.optimization_barrier(jnp.sum(weighted.astype(jnp.float32), axis=0))
    return (memory, norm_keys, peak, total, doc_pos[0], last_doc, jnp.zeros((), jnp.float32))

def emit(queries_blk, keys_blk, values_blk, in_gate, forget_pre, doc_pos, state):
    memory, norm_keys, top_in, total_in, first_in, last_in, empty_in = state
    scale = queries_blk.shape[1] ** (-0.5)
    logf = jax.nn.log_sigmoid(forget_pre)
    cum = jnp.cumsum(logf)
    length = queries_blk.shape[0]
    place = jnp.arange(length)
    keep = (place[:, None] >= place[None, :]) & (doc_pos[:, None] == doc_pos[None, :])
    exponent = jnp.where(keep, cum[:, None] - cum[None, :] + in_gate[None, :], far_low)
    usable = (doc_pos == last_in) & (empty_in < 0.5)
    carried = jnp.where(usable, cum + top_in, far_low)
    peak = jnp.maximum(carried, lax.optimization_barrier(jnp.max(exponent, axis=1)))
    scores = jnp.einsum('td,sd->ts', queries_blk.astype(jnp.float32), keys_blk.astype(jnp.float32)) * scale
    weights = jnp.where(keep, scores * jnp.exp(exponent - peak[:, None]), 0.0)
    inter = jnp.where(usable, jnp.exp(carried - peak), 0.0)
    query_wide = queries_blk.astype(jnp.float32)
    numer = jnp.dot(weights.astype(jnp.bfloat16), values_blk, preferred_element_type=jnp.float32)
    numer = numer + (inter * scale)[:, None] * jnp.dot(query_wide, memory, precision=lax.Precision.HIGHEST)
    denom = lax.optimization_barrier(jnp.sum(weights, axis=1)) + inter * scale * jnp.dot(query_wide, norm_keys, precision=lax.Precision.HIGHEST)
    return numer / jnp.maximum(jnp.abs(denom), 1.0)[:, None]

def combine(early, late):
    e_mem, e_keys, e_top, e_total, e_first, e_last, e_empty = early
    l_mem, l_keys, l_top, l_total, l_first, l_last, l_empty = late
    linked = (l_first == e_last) & (l_first == l_last) & (e_empty < 0.5)
    top = jnp.where(linked, jnp.maximum(l_top, e_top + l_total), l_top)
    early_part = jnp.where(linked, jnp.exp(jnp.minimum(e_top + l_total - top, 0.0)), 0.0)
    late_part = jnp.exp(l_top - top)
    joined = (early_part * e_mem + late_part * l_mem, early_part * e_keys + late_part * l_keys, top, e_total + l_total, jnp.where(e_empty > 0.5, l_first, e_first), l_last, jnp.zeros_like(l_empty))
    return tuple((jnp.where(l_empty > 0.5, a, b) for a, b in zip(early, joined)))

def run_direction(queries_h, keys_h, values_h, in_gate, forget_pre, doc_pos):

    def blocks(arr):
        return arr.reshape((N_SP, TOK_DEV) + arr.shape[1:])

    def step(state, pieces):
        q_blk, k_blk, v_blk, i_blk, f_blk, d_blk = pieces
        result = emit(q_blk, k_blk, v_blk, i_blk, f_blk, d_blk, state)
        return (combine(state, summarize(k_blk, v_blk, i_blk, f_blk, d_blk)), result)
    start = (jnp.zeros((DQK, DV), jnp.float32), jnp.zeros((DQK,), jnp.float32), jnp.full((), far_low, jnp.float32), jnp.zeros((), jnp.float32), jnp.full((), -1.0, jnp.float32), jnp.full((), -1.0, jnp.float32), jnp.ones((), jnp.float32))
    final, results = lax.scan(step, start, (blocks(queries_h), blocks(keys_h), blocks(values_h), blocks(in_gate), blocks(forget_pre), blocks(doc_pos)))
    return results.reshape(TOKENS, DV)

def reference(queries, keys, values, out_gate, input_gates, forget_gates, doc_ids, head_gain, w_out, resid, norm_gain, w_up, w_down):
    doc_pos = doc_ids.astype(jnp.float32)
    summed = jnp.zeros((TOKENS, D), jnp.float32)
    for head in range(HEADS):
        q_head = queries[:, head * DQK:(head + 1) * DQK]
        k_head = keys[:, head * DQK:(head + 1) * DQK]
        v_head = values[:, head * DV:(head + 1) * DV]
        forward = run_direction(q_head, k_head, v_head, input_gates[0, head], forget_gates[0, head], doc_pos)
        backward = run_direction(q_head[::-1], k_head[::-1], v_head[::-1], input_gates[1, head, ::-1], forget_gates[1, head, ::-1], doc_pos[::-1])[::-1]
        memory = forward + backward
        normed = memory * lax.rsqrt(lax.optimization_barrier(jnp.mean(memory * memory, axis=-1, keepdims=True)) + eps)
        gate = jax.nn.sigmoid(out_gate[:, head * DV:(head + 1) * DV].astype(jnp.float32))
        readout = (normed * head_gain[head * DV:(head + 1) * DV] * gate).astype(jnp.bfloat16)
        part = jnp.dot(readout, w_out[head * DV:(head + 1) * DV], preferred_element_type=jnp.float32).astype(jnp.bfloat16)
        summed = summed + lax.optimization_barrier(part).astype(jnp.float32)
    mixed = resid.astype(jnp.float32) + summed
    scaled = (mixed * lax.rsqrt(lax.optimization_barrier(jnp.mean(mixed * mixed, axis=-1, keepdims=True)) + eps) * norm_gain).astype(jnp.bfloat16)
    width = FF // HEADS

    def feed(rows_blk):
        hidden = jnp.square(jax.nn.relu(jnp.dot(rows_blk, w_up, preferred_element_type=jnp.float32))).astype(jnp.bfloat16)
        total = jnp.zeros((rows_blk.shape[0], D), jnp.float32)
        for group in range(HEADS):
            part = jnp.dot(hidden[:, group * width:(group + 1) * width], w_down[group * width:(group + 1) * width], preferred_element_type=jnp.float32).astype(jnp.bfloat16)
            total = total + lax.optimization_barrier(part).astype(jnp.float32)
        return total
    mixer = lax.map(feed, scaled.reshape(N_SP, TOK_DEV, D)).reshape(TOKENS, D)
    return (mixed + mixer).astype(jnp.bfloat16)
```

```python
import jax
import jax.numpy as jnp
from jax import lax
from jax.sharding import PartitionSpec as P

eps = 1e-06
far_low = -1e30
longest_doc = 3072


bf16 = jnp.bfloat16
f32 = jnp.float32


def dot(a, b):
    return jnp.dot(a, b, preferred_element_type=f32)


class Lines:
    def __init__(self):
        count = lax.axis_size("sp")
        self.pair = 2 if count % 2 == 0 else 1
        self.line = count // self.pair

    def along(self, value, step):
        table = [
            (z * self.pair + y, (z + step) * self.pair + y)
            for z in range(self.line)
            for y in range(self.pair)
            if 0 <= z + step < self.line
        ]
        return lax.ppermute(value, "sp", table)

    def across(self, value, valid):
        table = [
            (z * self.pair + y, z * self.pair + 1 - y)
            for z in range(self.line)
            if valid(z)
            for y in range(self.pair)
        ]
        return lax.ppermute(value, "sp", table)

    def order(self):
        place = lax.axis_index("sp")
        z, y = place // self.pair, place % self.pair
        sources = []
        for k in range(self.line):
            row = (z + self.line - k) % self.line
            sources.append(row * self.pair + y)
            if self.pair == 2:
                sources.append(row * self.pair + 1 - y)
        return jnp.stack(sources)

    def piece(self, source):
        place = lax.axis_index("sp")
        z, y = place // self.pair, place % self.pair
        k = (z + self.line - source // self.pair) % self.line
        return k * self.pair + (y + source) % self.pair

    def gather(self, own):
        n = self.line
        up, down = {}, {}
        up_side, down_side = {}, {}
        two = self.pair == 2
        own_side = self.across(own, lambda z: True) if two else None
        prev_up = prev_down = own
        for k in range(1, n):
            prev_up = up[k] = self.along(prev_up, 1)
            prev_down = down[k] = self.along(prev_down, -1)
            if two:
                up_side[k] = self.across(prev_up, lambda z: z >= k)
                down_side[k] = self.across(prev_down, lambda z: z + k < n)
        groups = [[own] + ([own_side] if two else [])]
        z = lax.axis_index("sp") // self.pair
        for k in range(1, n):
            below = z >= k
            group = [jnp.where(below, up[k], down[n - k])]
            if two:
                group.append(jnp.where(below, up_side[k], down_side[n - k]))
            groups.append(group)
        return groups


class Heads:
    def __init__(self):
        count = lax.axis_size("tp")
        self.core = 2 if count % 2 == 0 else 1
        self.far = count // self.core

    def swap(self, value):
        count = lax.axis_size("tp")
        return lax.ppermute(value, "tp", [(i, i ^ 1) for i in range(count)])

    def shift(self, value, step):
        table = [
            (x * self.core + c, ((x + step) % self.far) * self.core + c)
            for x in range(self.far)
            for c in range(self.core)
        ]
        return lax.ppermute(value, "tp", table)

    def gather(self, own):
        mine = [own] + [self.shift(own, r) for r in range(1, self.far)]
        if self.core == 1:
            return jnp.concatenate(mine)
        return jnp.concatenate(mine + [self.swap(block) for block in mine])

    def reduce(self, near, away):
        total = near.astype(f32)
        if away is not None:
            total = total + self.swap(away).astype(f32)
        out = total[0]
        for r in range(1, self.far):
            out = out + self.shift(total[r].astype(bf16), -r).astype(f32)
        return out


def local_part(scores, values, exponent, keep):
    top = jnp.max(jnp.where(keep, exponent, far_low), axis=1)
    weights = jnp.where(keep, scores * jnp.exp(exponent - top[:, None]), 0.0)
    return top, dot(weights.astype(bf16), values), jnp.sum(weights, axis=1)


def summary(keys, exponent):
    peak = jnp.max(exponent)
    weighted = (keys * jnp.exp(exponent - peak)[:, None]).astype(bf16)
    return weighted, jnp.sum(weighted.astype(f32), axis=0), peak


def incoming(memory, row, edge_doc, doc_here, sign, reach):
    count = lax.axis_size("sp")
    place = lax.axis_index("sp")
    depth = memory.shape[0]
    arrived = []
    for d in range(1, min(reach, count - 1) + 1):
        table = [(i, i + sign * d) for i in range(count) if 0 <= i + sign * d < count]
        arrived.append((lax.ppermute(row, "sp", table), lax.ppermute(memory, "sp", table)))
    passed = jnp.zeros((), f32)
    levels, linked = [], []
    for d, (got, _) in enumerate(arrived, 1):
        there = (place >= d) if sign > 0 else (place + d < count)
        joined = there & (got[depth + 2] == doc_here)
        levels.append(jnp.where(joined, got[depth] + passed, far_low))
        linked.append(joined)
        passed = passed + got[depth + 1]
    top = jnp.max(jnp.stack(levels))
    state = jnp.zeros(memory.shape, f32)
    norm = jnp.zeros((depth,), f32)
    for level, joined, (got, mem) in zip(levels, linked, arrived):
        share = jnp.where(joined, jnp.exp(level - top), 0.0)
        state = state + share * mem.astype(f32)
        norm = norm + share * got[:depth]
    return state.astype(bf16), norm, top, linked[0]


def one_head(queries, keys, values, in_gates, forget_pre, doc_pos, reach):
    length, depth = queries.shape
    scale = depth ** (-0.5)
    place = jnp.arange(length)
    logf = jax.nn.log_sigmoid(forget_pre)
    before = place[:, None] >= place[None, :]
    after = place[:, None] <= place[None, :]
    cum_f = jnp.sum(jnp.where(before, logf[0][None, :], 0.0), axis=1)
    cum_b = jnp.sum(jnp.where(after, logf[1][None, :], 0.0), axis=1)
    total_f, total_b = cum_f[length - 1], cum_b[0]
    first, last = doc_pos[0], doc_pos[length - 1]
    weighted_f, norm_f, peak_f = summary(
        keys, jnp.where(doc_pos == last, total_f - cum_f + in_gates[0], far_low)
    )
    weighted_b, norm_b, peak_b = summary(
        keys, jnp.where(doc_pos == first, total_b - cum_b + in_gates[1], far_low)
    )

    def own_state(weighted):
        return lax.dot_general(
            weighted, values, (((0,), (0,)), ((), ())), preferred_element_type=f32
        ).astype(bf16)

    pad = jnp.zeros((125,), f32)
    row_f = jnp.concatenate([norm_f, jnp.stack([peak_f, total_f, last]), pad])
    row_b = jnp.concatenate([norm_b, jnp.stack([peak_b, total_b, first]), pad])
    state_f, norm_in_f, top_f, has_f = incoming(own_state(weighted_f), row_f, last, first, 1, reach)
    state_b, norm_in_b, top_b, has_b = incoming(own_state(weighted_b), row_b, first, last, -1, reach)

    scores = (
        lax.dot_general(queries, keys, (((1,), (1,)), ((), ())), preferred_element_type=f32) * scale
    )
    same = doc_pos[:, None] == doc_pos[None, :]
    wide = queries.astype(f32)

    def finish(cum, gate, keep, state, norm_in, top_in, usable):
        exponent = cum[:, None] - cum[None, :] + gate[None, :]
        top, numer, denom = local_part(scores, values, exponent, keep)
        carried = jnp.where(usable, cum + top_in, far_low)
        peak = jnp.maximum(carried, top)
        local = jnp.exp(top - peak)
        inter = jnp.where(usable, jnp.exp(carried - peak), 0.0) * scale
        denom = local * denom + inter * jnp.sum(wide * norm_in[None, :], axis=1)
        under = 1.0 / jnp.maximum(jnp.abs(denom), 1.0)
        return (local * under)[:, None] * numer + (inter * under)[:, None] * dot(queries, state)

    return finish(
        cum_f, in_gates[0], before & same, state_f, norm_in_f, top_f, has_f & (doc_pos == first)
    ) + finish(
        cum_b, in_gates[1], after & same, state_b, norm_in_b, top_b, has_b & (doc_pos == last)
    )


def shards(
    queries,
    keys,
    values,
    out_gate,
    input_gates,
    forget_gates,
    doc_ids,
    head_gain,
    w_out,
    resid,
    norm_gain,
    w_up,
    w_down,
):
    length = queries.shape[0]
    heads = input_gates.shape[1]
    depth, width = queries.shape[1] // heads, values.shape[1] // heads
    lines, tps = Lines(), Heads()
    rows = resid.shape[0]
    doc_pos = doc_ids.astype(f32)
    reach = -(-longest_doc // length)
    ups = lines.gather(w_up)
    downs = lines.gather(w_down)
    order = lines.order()

    parts = []
    for h in range(heads):
        at_k, at_v = slice(h * depth, (h + 1) * depth), slice(h * width, (h + 1) * width)
        memory = one_head(
            queries[:, at_k],
            keys[:, at_k],
            values[:, at_v],
            input_gates[:, h],
            forget_gates[:, h],
            doc_pos,
            reach,
        )
        normed = memory * lax.rsqrt(jnp.mean(memory * memory, axis=-1, keepdims=True) + eps)
        gate = jax.nn.sigmoid(out_gate[:, at_v].astype(f32))
        parts.append((normed * head_gain[at_v] * gate).astype(bf16))
    readout = parts[0] if heads == 1 else jnp.concatenate(parts, axis=1)

    projected = dot(readout, w_out).astype(bf16).reshape(tps.far, tps.core, rows, -1)
    me = lax.axis_index("tp")
    x, c = me // tps.core, me % tps.core

    def for_core(core):
        picked = lax.dynamic_index_in_dim(projected, core, 1, False)
        return jnp.stack(
            [
                lax.dynamic_index_in_dim(picked, (x + tps.far - r) % tps.far, 0, False)
                for r in range(tps.far)
            ]
        )

    summed = tps.reduce(for_core(c), for_core(1 - c) if tps.core == 2 else None)
    mixed = resid.astype(f32) + summed
    factor = lax.rsqrt(jnp.mean(mixed * mixed, axis=-1, keepdims=True) + eps)
    scaled = (mixed * factor * norm_gain).astype(bf16)

    blocks = order.shape[0]
    deep = scaled.shape[1] // blocks
    turned = jnp.concatenate(
        [lax.dynamic_slice_in_dim(scaled, order[i] * deep, deep, 1) for i in range(blocks)], axis=1
    )
    up_full = jnp.concatenate([piece for group in ups for piece in group], axis=0)
    product = dot(tps.gather(turned), up_full)
    hidden = jnp.square(jax.nn.relu(product)).astype(bf16)

    bundle = max(1, len(downs) // 4)
    outs = []
    for at in range(0, len(downs), bundle):
        pieces = [piece for group in downs[at : at + bundle] for piece in group]
        part = dot(hidden, jnp.concatenate(pieces, axis=1)).astype(bf16)
        part = part.reshape(tps.core, tps.far, rows, -1)
        outs.append(tps.reduce(part[0], part[1] if tps.core == 2 else None))
    summed = jnp.concatenate(outs, axis=1)
    back = jnp.concatenate(
        [lax.dynamic_slice_in_dim(summed, lines.piece(i) * deep, deep, 1) for i in range(blocks)],
        axis=1,
    )
    return (mixed + back).astype(bf16)


def solution(mesh):
    in_specs = (
        P("sp", "tp"),
        P("sp", "tp"),
        P("sp", "tp"),
        P("sp", "tp"),
        P(None, "tp", "sp"),
        P(None, "tp", "sp"),
        P("sp"),
        P("tp"),
        P("tp", None),
        P(("sp", "tp"), None),
        P(),
        P("sp", "tp"),
        P("tp", "sp"),
    )
    out_specs = P(("sp", "tp"), None)
    return jax.shard_map(shards, mesh=mesh, in_specs=in_specs, out_specs=out_specs, check_vma=False)
```

```python
import jax
import jax.numpy as jnp
from jax import lax
from jax.sharding import PartitionSpec as P


eps = 1e-06
far_low = -1e30
longest_doc = 3072


bf16 = jnp.bfloat16
f32 = jnp.float32


def dot(a, b):
    return jnp.dot(a, b, preferred_element_type=f32)


class Lines:
    def __init__(self):
        count = lax.axis_size("sp")
        self.pair = 2 if count % 2 == 0 else 1
        self.line = count // self.pair

    def along(self, value, step):
        table = [
            (z * self.pair + y, (z + step) * self.pair + y)
            for z in range(self.line)
            for y in range(self.pair)
            if 0 <= z + step < self.line
        ]
        return lax.ppermute(value, "sp", table)

    def across(self, value, valid):
        table = [
            (z * self.pair + y, z * self.pair + 1 - y)
            for z in range(self.line)
            if valid(z)
            for y in range(self.pair)
        ]
        return lax.ppermute(value, "sp", table)

    def order(self):
        place = lax.axis_index("sp")
        z, y = place // self.pair, place % self.pair
        sources = []
        for k in range(self.line):
            row = (z + self.line - k) % self.line
            sources.append(row * self.pair + y)
            if self.pair == 2:
                sources.append(row * self.pair + 1 - y)
        return jnp.stack(sources)

    def piece(self, source):
        place = lax.axis_index("sp")
        z, y = place // self.pair, place % self.pair
        k = (z + self.line - source // self.pair) % self.line
        return k * self.pair + (y + source) % self.pair

    def gather(self, own):
        n = self.line
        up, down = {}, {}
        up_side, down_side = {}, {}
        two = self.pair == 2
        own_side = self.across(own, lambda z: True) if two else None
        prev_up = prev_down = own
        for k in range(1, n):
            prev_up = up[k] = self.along(prev_up, 1)
            prev_down = down[k] = self.along(prev_down, -1)
            if two:
                up_side[k] = self.across(prev_up, lambda z: z >= k)
                down_side[k] = self.across(prev_down, lambda z: z + k < n)
        groups = [[own] + ([own_side] if two else [])]
        z = lax.axis_index("sp") // self.pair
        for k in range(1, n):
            below = z >= k
            group = [jnp.where(below, up[k], down[n - k])]
            if two:
                group.append(jnp.where(below, up_side[k], down_side[n - k]))
            groups.append(group)
        return groups


class Heads:
    def __init__(self):
        count = lax.axis_size("tp")
        self.core = 2 if count % 2 == 0 else 1
        self.far = count // self.core

    def swap(self, value):
        count = lax.axis_size("tp")
        return lax.ppermute(value, "tp", [(i, i ^ 1) for i in range(count)])

    def shift(self, value, step):
        table = [
            (x * self.core + c, ((x + step) % self.far) * self.core + c)
            for x in range(self.far)
            for c in range(self.core)
        ]
        return lax.ppermute(value, "tp", table)

    def gather(self, own):
        mine = [own] + [self.shift(own, r) for r in range(1, self.far)]
        if self.core == 1:
            return jnp.concatenate(mine)
        return jnp.concatenate(mine + [self.swap(block) for block in mine])

    def reduce(self, near, away):
        total = near.astype(f32)
        if away is not None:
            total = total + self.swap(away).astype(f32)
        out = total[0]
        for r in range(1, self.far):
            out = out + self.shift(total[r].astype(bf16), -r).astype(f32)
        return out


def local_part(scores, values, exponent, keep):
    top = jnp.max(jnp.where(keep, exponent, far_low), axis=1)
    weights = jnp.where(keep, scores * jnp.exp(exponent - top[:, None]), 0.0)
    return top, dot(weights.astype(bf16), values), jnp.sum(weights, axis=1)


def summary(keys, exponent):
    peak = jnp.max(exponent)
    weighted = (keys * jnp.exp(exponent - peak)[:, None]).astype(bf16)
    return weighted, jnp.sum(weighted.astype(f32), axis=0), peak


def split_row(row, width):
    terms, rest = [], row
    for _ in range(3):
        term = lax.reduce_precision(rest, 8, 7)
        rest = rest - term
        terms.append(term.astype(bf16))
    lines = -(-row.shape[0] // width)
    table = jnp.stack([jnp.pad(t, (0, lines * width - t.shape[0])) for t in terms])
    table = table.reshape(3 * lines, width)
    return jnp.pad(table, ((0, -(3 * lines) % 16), (0, 0)))


def join_row(table, size):
    lines = -(-size // table.shape[1])
    terms = table[: 3 * lines].astype(f32).reshape(3, -1)
    return (terms[0] + terms[1] + terms[2])[:size]


def incoming(memory, row, doc_here, sign, reach):
    count = lax.axis_size("sp")
    place = lax.axis_index("sp")
    depth, width = memory.shape
    sent = jnp.concatenate([memory, split_row(row, width)])
    arrived = []
    for d in range(1, min(reach, count - 1) + 1):
        table = [(i, i + sign * d) for i in range(count) if 0 <= i + sign * d < count]
        got = lax.ppermute(sent, "sp", table)
        arrived.append((join_row(got[depth:], row.shape[0]), got[:depth]))
    passed = jnp.zeros((), f32)
    levels, linked = [], []
    for d, (got, _) in enumerate(arrived, 1):
        there = (place >= d) if sign > 0 else (place + d < count)
        joined = there & (got[depth + 2] == doc_here)
        levels.append(jnp.where(joined, got[depth] + passed, far_low))
        linked.append(joined)
        passed = passed + got[depth + 1]
    top = jnp.max(jnp.stack(levels))
    state = jnp.zeros(memory.shape, f32)
    norm = jnp.zeros((depth,), f32)
    for level, joined, (got, mem) in zip(levels, linked, arrived):
        share = jnp.where(joined, jnp.exp(level - top), 0.0)
        state = state + share * mem.astype(f32)
        norm = norm + share * got[:depth]
    return state.astype(bf16), norm, top, linked[0]


def one_head(queries, keys, values, in_gates, forget_pre, doc_pos, reach):
    length, depth = queries.shape
    scale = depth ** (-0.5)
    place = jnp.arange(length)
    logf = jax.nn.log_sigmoid(forget_pre)
    before = place[:, None] >= place[None, :]
    after = place[:, None] <= place[None, :]
    cum_f = jnp.sum(jnp.where(before, logf[0][None, :], 0.0), axis=1)
    cum_b = jnp.sum(jnp.where(after, logf[1][None, :], 0.0), axis=1)
    total_f, total_b = cum_f[length - 1], cum_b[0]
    first, last = doc_pos[0], doc_pos[length - 1]
    weighted_f, norm_f, peak_f = summary(
        keys, jnp.where(doc_pos == last, total_f - cum_f + in_gates[0], far_low)
    )
    weighted_b, norm_b, peak_b = summary(
        keys, jnp.where(doc_pos == first, total_b - cum_b + in_gates[1], far_low)
    )

    def own_state(weighted):
        return lax.dot_general(
            weighted, values, (((0,), (0,)), ((), ())), preferred_element_type=f32
        ).astype(bf16)

    pad = jnp.zeros((125,), f32)
    row_f = jnp.concatenate([norm_f, jnp.stack([peak_f, total_f, last]), pad])
    row_b = jnp.concatenate([norm_b, jnp.stack([peak_b, total_b, first]), pad])
    state_f, norm_in_f, top_f, has_f = incoming(own_state(weighted_f), row_f, first, 1, reach)
    state_b, norm_in_b, top_b, has_b = incoming(own_state(weighted_b), row_b, last, -1, reach)

    scores = (
        lax.dot_general(queries, keys, (((1,), (1,)), ((), ())), preferred_element_type=f32) * scale
    )
    same = doc_pos[:, None] == doc_pos[None, :]
    wide = queries.astype(f32)

    def finish(cum, gate, keep, state, norm_in, top_in, usable):
        exponent = cum[:, None] - cum[None, :] + gate[None, :]
        top, numer, denom = local_part(scores, values, exponent, keep)
        carried = jnp.where(usable, cum + top_in, far_low)
        peak = jnp.maximum(carried, top)
        local = jnp.exp(top - peak)
        inter = jnp.where(usable, jnp.exp(carried - peak), 0.0) * scale
        denom = local * denom + inter * jnp.sum(wide * norm_in[None, :], axis=1)
        under = 1.0 / jnp.maximum(jnp.abs(denom), 1.0)
        return (local * under)[:, None] * numer + (inter * under)[:, None] * dot(queries, state)

    return finish(
        cum_f, in_gates[0], before & same, state_f, norm_in_f, top_f, has_f & (doc_pos == first)
    ) + finish(
        cum_b, in_gates[1], after & same, state_b, norm_in_b, top_b, has_b & (doc_pos == last)
    )


def pack(w_up, w_down):
    wide = w_down.shape[1]
    count = w_up.shape[1] // wide
    tiles = [w_down[i * wide : (i + 1) * wide] for i in range(count)]
    return jnp.concatenate([w_up, jnp.concatenate(tiles, axis=1)])


def unpack(table, wide):
    count = table.shape[1] // wide
    return jnp.concatenate([table[:, i * wide : (i + 1) * wide] for i in range(count)])


def layer(
    queries,
    keys,
    values,
    out_gate,
    input_gates,
    forget_gates,
    doc_ids,
    head_gain,
    w_out,
    resid,
    norm_gain,
    w_up,
    w_down,
):
    length = queries.shape[0]
    heads = input_gates.shape[1]
    depth, width = queries.shape[1] // heads, values.shape[1] // heads
    lines, tps = Lines(), Heads()
    rows = resid.shape[0]
    doc_pos = doc_ids.astype(f32)
    reach = -(-longest_doc // length)
    deep_up, wide_down = w_up.shape[0], w_down.shape[1]
    groups = lines.gather(pack(w_up, w_down))
    ups = [[piece[:deep_up] for piece in group] for group in groups]
    downs = [[unpack(piece[deep_up:], wide_down) for piece in group] for group in groups]
    order = lines.order()

    parts = []
    for h in range(heads):
        at_k, at_v = slice(h * depth, (h + 1) * depth), slice(h * width, (h + 1) * width)
        memory = one_head(
            queries[:, at_k],
            keys[:, at_k],
            values[:, at_v],
            input_gates[:, h],
            forget_gates[:, h],
            doc_pos,
            reach,
        )
        normed = memory * lax.rsqrt(jnp.mean(memory * memory, axis=-1, keepdims=True) + eps)
        gate = jax.nn.sigmoid(out_gate[:, at_v].astype(f32))
        parts.append((normed * head_gain[at_v] * gate).astype(bf16))
    readout = parts[0] if heads == 1 else jnp.concatenate(parts, axis=1)

    projected = dot(readout, w_out).astype(bf16).reshape(tps.far, tps.core, rows, -1)
    me = lax.axis_index("tp")
    x, c = me // tps.core, me % tps.core

    def for_core(core):
        picked = lax.dynamic_index_in_dim(projected, core, 1, False)
        return jnp.stack(
            [
                lax.dynamic_index_in_dim(picked, (x + tps.far - r) % tps.far, 0, False)
                for r in range(tps.far)
            ]
        )

    summed = tps.reduce(for_core(c), for_core(1 - c) if tps.core == 2 else None)
    mixed = resid.astype(f32) + summed
    factor = lax.rsqrt(jnp.mean(mixed * mixed, axis=-1, keepdims=True) + eps)
    scaled = (mixed * factor * norm_gain).astype(bf16)

    blocks = order.shape[0]
    deep = scaled.shape[1] // blocks
    turned = jnp.concatenate(
        [lax.dynamic_slice_in_dim(scaled, order[i] * deep, deep, 1) for i in range(blocks)], axis=1
    )
    up_full = jnp.concatenate([piece for group in ups for piece in group], axis=0)
    product = dot(tps.gather(turned), up_full)
    hidden = jnp.square(jax.nn.relu(product)).astype(bf16)

    bundle = max(1, len(downs) // 4)
    outs = []
    for at in range(0, len(downs), bundle):
        pieces = [piece for group in downs[at : at + bundle] for piece in group]
        part = dot(hidden, jnp.concatenate(pieces, axis=1)).astype(bf16)
        part = part.reshape(tps.core, tps.far, rows, -1)
        outs.append(tps.reduce(part[0], part[1] if tps.core == 2 else None))
    summed = jnp.concatenate(outs, axis=1)
    back = jnp.concatenate(
        [lax.dynamic_slice_in_dim(summed, lines.piece(i) * deep, deep, 1) for i in range(blocks)],
        axis=1,
    )
    return (mixed + back).astype(bf16)


def solution(mesh):
    in_specs = (
        P("sp", "tp"),
        P("sp", "tp"),
        P("sp", "tp"),
        P("sp", "tp"),
        P(None, "tp", "sp"),
        P(None, "tp", "sp"),
        P("sp"),
        P("tp"),
        P("tp", None),
        P(("sp", "tp"), None),
        P(),
        P("sp", "tp"),
        P("tp", "sp"),
    )
    out_specs = P(("sp", "tp"), None)
    return jax.shard_map(layer, mesh=mesh, in_specs=in_specs, out_specs=out_specs, check_vma=False)
```
